32 devices in a mesh: sp: 8 (over z, x), tp: 4 (over y, core).
Axes of the slice: x: 2, y: 2, z: 4, core: 2. Of those that a mesh axis runs over, the one named last changes fastest.
Arguments:
- tokens: bfloat16 [4096, 2048], P(('sp', 'tp')), may hold values from -64 to 64
- query_weight: bfloat16 [2048, 2048], P(None, 'tp'), may hold values from -0.125 to 0.125
- key_weight: bfloat16 [2048, 2048], P(None, 'tp'), may hold values from -0.125 to 0.125
- value_weight: bfloat16 [2048, 2048], P(None, 'tp'), may hold values from -0.125 to 0.125
- gate_weight: bfloat16 [2048, 2048], P(None, 'tp'), may hold values from -0.125 to 0.125
- forget_weight: bfloat16 [2048, 16], replicated, may hold values from -0.125 to 0.125
- forget_bias: float32 [16], replicated, as said below
- out_weight: bfloat16 [2048, 2048], replicated, may hold values from -0.125 to 0.125
Outputs:
- mixed: bfloat16 [4096, 2048], P(('sp', 'tp'))
The draws below stay inside these ranges and needn't reach their ends.
Inputs may be any that keep to these rules, and one draw needn't show every extreme that they name: `forget_bias`: every head's forget bias is at least 4.
All inputs are finite; a program needn't handle non-finite values.
Results may differ from the reference program's by a relative error of at most 0.015.
The reference program's roundings to bfloat16 on the way (of `queries`, `keys`, `values` and `attended`) count: a program that leaves them out, or rounds other values in their place, can miss the bound.
Values may be sent and summed in bfloat16 or wider, within the bound.
A program may use at most 128 MiB of HBM per device.

```python
import math
import jax
import jax.numpy as jnp
from jax import lax

D = 2048
HEADS = 16
HEAD_DIM = 128
TOK_DEV = 512
SEQ = 4096


def draw_tokens(key, part):
    keys = jax.random.split(jax.random.fold_in(key, 11), 5)
    span = max(TOK_DEV // 4, 1)
    blocks = SEQ // span
    base = jnp.clip(jax.random.normal(keys[0], (SEQ, D), jnp.float32), -4.0, 4.0)
    shifts = 0.7 * jnp.clip(jax.random.normal(keys[1], (blocks, D), jnp.float32), -2.0, 2.0)
    scales = jnp.exp(jax.random.uniform(keys[2], (blocks, 1), jnp.float32, jnp.log(0.5), jnp.log(2.0)))
    field = (base.reshape(blocks, span, D) + shifts[:, None, :]) * scales[:, None, :]
    field = field.reshape(SEQ, D)
    return jnp.clip(field, -64.0, 64.0).astype(jnp.bfloat16)


def draw_forget_bias(key, part):
    keys = jax.random.split(jax.random.fold_in(key, 23), 2)
    order = jax.random.permutation(keys[0], HEADS)
    fast_count = HEADS // 2
    fast = (order < fast_count).astype(jnp.float32)
    spread = jax.random.uniform(keys[1], (HEADS,), jnp.float32)
    slow_bias = jnp.log(jnp.float32(SEQ)) + 1.0 + spread
    fast_bias = 4.0 + 1.5 * spread
    return fast * fast_bias + (1.0 - fast) * slow_bias


def shard_levels(key, extent, shards, smallest, top_value):
    factor_of = 1.0
    for axis_at, shards_of in shards:
        steps = jax.random.uniform(jax.random.fold_in(jax.random.fold_in(key, 6), axis_at), (shards_of,), jnp.float32, smallest / len(shards), top_value / len(shards))
        factor_of = factor_of * jnp.repeat(jnp.exp(steps), extent[axis_at] // shards_of).reshape((-1,) + (1,) * (len(extent) - 1 - axis_at))
    return factor_of


def noise(stream_key, dims, width, bound, pieces=(), held_as=jnp.bfloat16):
    factor_of = shard_levels(stream_key, dims, pieces, -0.22, 0.18) if pieces else 1.0
    drawn = jax.random.normal(stream_key, dims, jnp.float32) * width * factor_of
    return jnp.minimum(jnp.maximum(drawn, -bound), bound).astype(held_as)


def setup_inputs(seed: int = 0) -> dict:
    streams_of = jax.random.split(jax.random.key(seed), 9)
    tokens = draw_tokens(jax.random.fold_in(streams_of[8], 71), 0)
    query_weight = noise(streams_of[1], (D, D), D ** -0.5, 0.125, ((1, 4),))
    key_weight = noise(streams_of[2], (D, D), D ** -0.5, 0.125, ((1, 4),))
    value_weight = noise(streams_of[3], (D, D), D ** -0.5, 0.125, ((1, 4),))
    gate_weight = noise(streams_of[4], (D, D), D ** -0.5, 0.125, ((1, 4),))
    forget_weight = noise(streams_of[5], (D, HEADS), D ** -0.5, 0.125)
    forget_bias = draw_forget_bias(jax.random.fold_in(streams_of[8], 71), 0)
    out_weight = noise(streams_of[7], (D, D), D ** -0.5, 0.125)
    return {"tokens": tokens, "query_weight": query_weight, "key_weight": key_weight, "value_weight": value_weight, "gate_weight": gate_weight, "forget_weight": forget_weight, "forget_bias": forget_bias, "out_weight": out_weight}


def reference(tokens, query_weight, key_weight, value_weight, gate_weight, forget_weight, forget_bias, out_weight):
    scale = HEAD_DIM ** -0.5
    queries = (jnp.dot(tokens, query_weight, preferred_element_type=jnp.float32) * scale).astype(jnp.bfloat16)
    keys = jnp.dot(tokens, key_weight, preferred_element_type=jnp.float32).astype(jnp.bfloat16)
    values = jnp.dot(tokens, value_weight, preferred_element_type=jnp.float32).astype(jnp.bfloat16)
    gate = jax.nn.sigmoid(jnp.dot(tokens, gate_weight, preferred_element_type=jnp.float32))
    forget_log = jax.nn.log_sigmoid(jnp.dot(tokens, forget_weight, preferred_element_type=jnp.float32) + forget_bias)
    cumul = jnp.cumsum(forget_log.T, axis=1)
    span = math.gcd(SEQ, 512)
    blocks = SEQ // span
    positions = jnp.arange(SEQ, dtype=jnp.int32)

    def one_head(args):
        head_q, head_k, head_v, head_c = args
        query_blocks = head_q.reshape(blocks, span, HEAD_DIM)
        cum_blocks = head_c.reshape(blocks, span)
        pos_blocks = positions.reshape(blocks, span)

        def one_block(inner):
            block_q, block_c, block_p = inner
            scores = jnp.dot(block_q, head_k.T, preferred_element_type=jnp.float32)
            scores = scores + block_c[:, None] - head_c[None, :]
            scores = jnp.where(positions[None, :] <= block_p[:, None], scores, -jnp.inf)
            top = jnp.max(scores, axis=1, keepdims=True)
            weights = jnp.exp(scores - top)
            denom = jnp.sum(weights, axis=1, keepdims=True)
            return jnp.dot(weights.astype(jnp.bfloat16), head_v, preferred_element_type=jnp.float32) / denom

        return lax.map(one_block, (query_blocks, cum_blocks, pos_blocks)).reshape(SEQ, HEAD_DIM)

    split_q = queries.reshape(SEQ, HEADS, HEAD_DIM).transpose(1, 0, 2)
    split_k = keys.reshape(SEQ, HEADS, HEAD_DIM).transpose(1, 0, 2)
    split_v = values.reshape(SEQ, HEADS, HEAD_DIM).transpose(1, 0, 2)
    heads_out = lax.map(one_head, (split_q, split_k, split_v, cumul))
    heads_out = heads_out.transpose(1, 0, 2).reshape(SEQ, D)
    attended = (heads_out * gate).astype(jnp.bfloat16)
    return jnp.dot(attended, out_weight, preferred_element_type=jnp.float32).astype(jnp.bfloat16)
```

```python
import functools

import jax
import jax.numpy as jnp
from jax import lax
from jax.experimental import pallas as pl
from jax.experimental.pallas import tpu as pltpu
from jax.sharding import PartitionSpec as P

HEAD_DIM = 128
CORES = 2
MESH = pl.DeviceIdType.MESH
F32 = jnp.float32
BF16 = jnp.bfloat16


def kernel(
    dims,
    x_hbm, wq_hbm, wk_hbm, wv_hbm, wg_hbm, fw_ref, fb_ref, wo_hbm,
    out_ref,
    tok, wbuf, wo, kvs, qs_, gs, fs, kvd, qd, fd, crow, obuf, oin, gin, att,
    m_ref, l_ref, acc_ref,
    load_sem, tok_send, tok_recv, tok_fwd,
    kv_send, f_send, q_send, g_send, kv_fwd, f_fwd,
    kv_recv, f_recv, q_recv, g_recv, o_send, o_recv,
):
    S, T, td, D, hd = dims
    H = T * hd
    rows = T * td
    ny = T // CORES
    gr = CORES * td
    hp = CORES * hd
    cph = S // hp
    G = CORES * cph
    seq = S * rows
    ng = S * ny
    ch = seq // (2 * G)
    qt = min(512, ch)
    kb = qt
    width = hd * HEAD_DIM
    s = lax.axis_index("sp")
    t = lax.axis_index("tp")
    y = t // CORES
    c = t % CORES
    peer = y * CORES + (1 - c)

    def remote(src, dst, ssem, rsem, ds, dt):
        return pltpu.make_async_remote_copy(
            src_ref=src, dst_ref=dst, send_sem=ssem, recv_sem=rsem,
            device_id={"sp": ds, "tp": dt}, device_id_type=MESH,
        )

    def send(src, dst, ssem, rsem, ds, dt):
        mine = jnp.logical_and(ds == s, dt == t)

        @pl.when(mine)
        def _():
            pltpu.make_async_copy(src, dst, rsem).start()

        @pl.when(jnp.logical_not(mine))
        def _():
            remote(src, dst, ssem, rsem, ds, dt).start()

    def sent(src, dst, ssem, rsem, ds, dt):
        mine = jnp.logical_and(ds == s, dt == t)

        @pl.when(jnp.logical_not(mine))
        def _():
            remote(src, dst, ssem, rsem, ds, dt).wait_send()

    def arrived(dst, rsem):
        pltpu.make_async_copy(dst, dst, rsem).wait()

    def piece(i):
        return tok.at[pl.ds(pl.multiple_of(i * td, td), td)]

    own = pltpu.make_async_copy(x_hbm, piece(t), load_sem.at[0])
    own.start()
    loads = []
    for i, w in enumerate((wk_hbm, wv_hbm, wq_hbm, wg_hbm)):
        loads.append(pltpu.make_async_copy(w, wbuf.at[i], load_sem.at[1 + i]))
    loads.append(pltpu.make_async_copy(wo_hbm, wo, load_sem.at[5]))
    for ld in loads:
        ld.start()
    own.wait()
    tok_copies = []
    for dy in range(1, ny):
        dt = ((y + dy) % ny) * CORES + c
        tok_copies.append(remote(piece(t), piece(t), tok_send.at[dy], tok_recv.at[t], s, dt))
    tok_copies.append(remote(piece(t), piece(t), tok_send.at[0], tok_recv.at[t], s, peer))
    for cp in tok_copies:
        cp.start()
    arrived(piece(peer), tok_recv.at[peer])

    lane = lax.broadcasted_iota(jnp.int32, (H, gr), 1)

    def q_place(b):
        start = b * gr
        ci = start // ch
        late = ci // G
        r = ci + late * (2 * G - 1 - 2 * ci)
        return r, pl.multiple_of(late * ch + start % ch, gr)

    def kv_args(dy, yg, j, m):
        b = s * ny + yg
        jj = c * hd + j
        at = (dy * hd + j) * cph + m
        dst_s = jj * cph + m
        dst_t = y * CORES + s % CORES
        base = pl.multiple_of(yg * gr, gr)
        gbase = pl.multiple_of(b * gr, gr)
        return (
            (kvs.at[j, pl.ds(base, gr)], kvd.at[pl.ds(gbase, gr)], kv_send.at[at], kv_recv.at[b], dst_s, dst_t),
            (fs.at[dy, t * hd + j], fd.at[b], f_send.at[at], f_recv.at[b], dst_s, dst_t),
        )

    def q_args(dy, yg, j):
        b = s * ny + yg
        jj = c * hd + j
        r, pos = q_place(b)
        base = pl.multiple_of(yg * gr, gr)
        return (
            qs_.at[j, pl.ds(base, gr)], qd.at[pl.ds(pos, gr)], q_send.at[dy * hd + j],
            q_recv.at[pos // gr], jj * cph + r // CORES, y * CORES + r % CORES,
        )

    def g_args(dt):
        return (
            gs.at[:, pl.ds(pl.multiple_of(dt * td, td), td)], gin.at[pl.ds(t * hd, hd)],
            g_send.at[dt], g_recv.at[t], s, dt,
        )

    for dy in range(ny):
        yg = (y + dy) % ny
        base = pl.multiple_of(yg * gr, gr)
        if dy > 0:
            got = yg * CORES + c
            other = yg * CORES + 1 - c
            arrived(piece(got), tok_recv.at[got])
            remote(piece(got), piece(got), tok_fwd.at[dy], tok_recv.at[got], s, peer).start()
            arrived(piece(other), tok_recv.at[other])
        x = tok[pl.ds(base, gr), :]
        if dy == 0:
            loads[0].wait()
        prod = jnp.dot(x, wbuf[0], preferred_element_type=F32)
        for j in range(hd):
            kvs[j, pl.ds(base, gr), 0:HEAD_DIM] = prod[:, j * HEAD_DIM : (j + 1) * HEAD_DIM].astype(BF16)
        if dy == 0:
            loads[1].wait()
        prod = jnp.dot(x, wbuf[1], preferred_element_type=F32)
        for j in range(hd):
            kvs[j, pl.ds(base, gr), HEAD_DIM:] = prod[:, j * HEAD_DIM : (j + 1) * HEAD_DIM].astype(BF16)
        logit = lax.dot_general(
            fw_ref[...], x, (((1,), (1,)), ((), ())), preferred_element_type=F32
        ) + fb_ref[:, 0:1]
        logs = jnp.minimum(logit, 0.0) - jnp.log1p(jnp.exp(-jnp.abs(logit)))
        step = 1
        while step < gr:
            logs = logs + jnp.where(lane >= step, pltpu.roll(logs, step, 1), 0.0)
            step *= 2
        for h in range(H):
            fs[dy, h] = jnp.broadcast_to(logs[h : h + 1, :], (8, gr))
        for j in range(hd):
            for m in range(cph):
                kv, f = kv_args(dy, yg, j, m)
                send(*kv)
                send(*f)
        if dy == 0:
            loads[2].wait()
        prod = jnp.dot(x, wbuf[2], preferred_element_type=F32) * HEAD_DIM ** (-0.5)
        for j in range(hd):
            qs_[j, pl.ds(base, gr)] = prod[:, j * HEAD_DIM : (j + 1) * HEAD_DIM].astype(BF16)
        for j in range(hd):
            send(*q_args(dy, yg, j))
        if dy == 0:
            loads[3].wait()
        prod = jax.nn.sigmoid(jnp.dot(x, wbuf[3], preferred_element_type=F32))
        for j in range(hd):
            gs[j, pl.ds(base, gr)] = prod[:, j * HEAD_DIM : (j + 1) * HEAD_DIM]
        for e in range(CORES):
            send(*g_args(yg * CORES + e))

    def fwd_args(b):
        gbase = pl.multiple_of(b * gr, gr)
        at = (b // ny) // CORES * ny + b % ny
        blk = kvd.at[pl.ds(gbase, gr)]
        return (
            (blk, blk, kv_fwd.at[at], kv_recv.at[b], s, peer),
            (fd.at[b], fd.at[b], f_fwd.at[at], f_recv.at[b], s, peer),
        )

    def fwd_block(i, parity):
        return ((i // ny) * CORES + parity) * ny + i % ny

    def forward(i, carry):
        b = fwd_block(i, c)
        kv, f = fwd_args(b)
        arrived(f[0], f_recv.at[b])
        remote(*f).start()
        arrived(kv[0], kv_recv.at[b])
        remote(*kv).start()
        return carry

    lax.fori_loop(0, ng // CORES, forward, 0)

    def collect(i, carry):
        b = fwd_block(i, 1 - c)
        kv, f = fwd_args(b)
        arrived(f[0], f_recv.at[b])
        arrived(kv[0], kv_recv.at[b])
        return carry

    lax.fori_loop(0, ng // CORES, collect, 0)

    def q_wait(i, carry):
        arrived(qd.at[pl.ds(pl.multiple_of(i * gr, gr), gr)], q_recv.at[i])
        return carry

    lax.fori_loop(0, 2 * ch // gr, q_wait, 0)

    def chain(b, offset):
        blk = fd[b] + offset
        crow[:, pl.ds(pl.multiple_of(b * gr, gr), gr)] = blk
        return blk[:, gr - 1 : gr]

    lax.fori_loop(0, ng, chain, jnp.zeros((8, 1), F32))

    r = (s % cph) * CORES + c
    head = y * hp + s // cph
    above = lax.broadcasted_iota(jnp.int32, (qt, kb), 1) > lax.broadcasted_iota(jnp.int32, (qt, kb), 0)

    def o_args(half, u):
        ci = r if half == 0 else 2 * G - 1 - r
        token = ci * ch + u * td
        at = half * (ch // td) + u
        return (
            obuf.at[pl.ds(pl.multiple_of(half * ch + u * td, td), td)], oin.at[head],
            o_send.at[at], o_recv.at[head], token // rows, (token % rows) // td,
        )

    for half in range(2):
        ci = r if half == 0 else 2 * G - 1 - r
        for tile in range(ch // qt):
            at = half * ch + tile * qt
            q0 = pl.multiple_of(ci * ch + tile * qt, qt)
            q = qd[at : at + qt, :]
            cq = crow[:, pl.ds(q0, qt)]
            c0 = cq[0:1, 0:1]
            cqc = (cq - c0).T[:, 0:1]
            m_ref[...] = jnp.full(m_ref.shape, -1e30, F32)
            l_ref[...] = jnp.zeros(l_ref.shape, F32)
            acc_ref[...] = jnp.zeros(acc_ref.shape, F32)

            def absorb(kblk, masked, q=q, c0=c0, cqc=cqc):
                k0 = pl.multiple_of(kblk * kb, kb)
                scores = lax.dot_general(
                    q, kvd[pl.ds(k0, kb), 0:HEAD_DIM], (((1,), (1,)), ((), ())),
                    preferred_element_type=F32,
                )
                scores = scores + (c0 - crow[0:1, pl.ds(k0, kb)])
                if masked:
                    scores = jnp.where(above, -jnp.inf, scores)
                best = m_ref[:, 0:1]
                top = jnp.maximum(best, jnp.max(scores, axis=1, keepdims=True) + cqc)
                factor = jnp.exp(best - top)
                weights = jnp.exp(scores - (top - cqc))
                part = weights[:, 0:128]
                for i in range(1, kb // 128):
                    part = part + weights[:, i * 128 : (i + 1) * 128]
                l_ref[...] = l_ref[...] * factor + part
                acc_ref[...] = acc_ref[...] * factor + jnp.dot(
                    weights.astype(BF16), kvd[pl.ds(k0, kb), HEAD_DIM:], preferred_element_type=F32
                )
                m_ref[...] = jnp.broadcast_to(top, m_ref.shape)

            full = q0 // kb

            def full_step(i, carry):
                absorb(i, False)
                return carry

            lax.fori_loop(0, full, full_step, 0)
            absorb(full, True)
            total = jnp.sum(l_ref[...], axis=1, keepdims=True)
            obuf[at : at + qt, :] = (acc_ref[...] / total).astype(BF16)
            for u in range(qt // td):
                send(*o_args(half, tile * (qt // td) + u))

    def g_wait(i, carry):
        arrived(gin.at[pl.ds(i * hd, hd)], g_recv.at[i])
        return carry

    lax.fori_loop(0, T, g_wait, 0)
    loads[4].wait()
    for h in range(H):
        arrived(oin.at[h], o_recv.at[h])
        att[:, h * HEAD_DIM : (h + 1) * HEAD_DIM] = (oin[h].astype(F32) * gin[h]).astype(BF16)
    cols = 512
    for n in range(D // cols):
        out_ref[:, n * cols : (n + 1) * cols] = jnp.dot(
            att[...], wo[:, n * cols : (n + 1) * cols], preferred_element_type=F32
        ).astype(BF16)

    for cp in tok_copies:
        cp.wait_send()
    for dy in range(ny):
        yg = (y + dy) % ny
        if dy > 0:
            got = yg * CORES + c
            remote(piece(got), piece(got), tok_fwd.at[dy], tok_recv.at[got], s, peer).wait_send()
        for j in range(hd):
            for m in range(cph):
                kv, f = kv_args(dy, yg, j, m)
                sent(*kv)
                sent(*f)
            sent(*q_args(dy, yg, j))
        for e in range(CORES):
            sent(*g_args(yg * CORES + e))

    def fwd_done(i, carry):
        kv, f = fwd_args(fwd_block(i, c))
        remote(*f).wait_send()
        remote(*kv).wait_send()
        return carry

    lax.fori_loop(0, ng // CORES, fwd_done, 0)
    for half in range(2):
        for u in range(ch // td):
            sent(*o_args(half, u))


def body(tokens, wq, wk, wv, wg, fw, fb, wo, *, S, T):
    td, D = tokens.shape
    width = wq.shape[1]
    hd = width // HEAD_DIM
    H = T * hd
    rows = T * td
    ny = T // CORES
    gr = CORES * td
    hp = CORES * hd
    cph = S // hp
    G = CORES * cph
    seq = S * rows
    ng = S * ny
    ch = seq // (2 * G)
    qt = min(512, ch)
    dma = pltpu.SemaphoreType.DMA
    vmem = pltpu.VMEM
    any_ = pl.BlockSpec(memory_space=pl.ANY)
    vm = pl.BlockSpec(memory_space=pltpu.VMEM)
    scratch = [
        vmem((rows, D), BF16), vmem((4, D, width), BF16), vmem((D, D), BF16),
        vmem((hd, rows, 2 * HEAD_DIM), BF16), vmem((hd, rows, HEAD_DIM), BF16),
        vmem((hd, rows, HEAD_DIM), F32), vmem((ny, H, 8, gr), F32),
        vmem((seq, 2 * HEAD_DIM), BF16), vmem((2 * ch, HEAD_DIM), BF16),
        vmem((ng, 8, gr), F32), vmem((8, seq), F32), vmem((2 * ch, HEAD_DIM), BF16),
        vmem((H, td, HEAD_DIM), BF16), vmem((H, td, HEAD_DIM), F32), vmem((td, D), BF16),
        vmem((qt, 128), F32), vmem((qt, 128), F32), vmem((qt, HEAD_DIM), F32),
        dma((6,)), dma((ny,)), dma((T,)), dma((ny,)),
        dma((ny * hd * cph,)), dma((ny * hd * cph,)), dma((ny * hd,)), dma((T,)),
        dma((ng // CORES,)), dma((ng // CORES,)),
        dma((ng,)), dma((ng,)), dma((2 * ch // gr,)), dma((T,)), dma((2 * ch // td,)), dma((H,)),
    ]
    return pl.pallas_call(
        functools.partial(kernel, (S, T, td, D, hd)),
        out_shape=jax.ShapeDtypeStruct((td, D), BF16),
        in_specs=[any_, any_, any_, any_, any_, vm, vm, any_],
        out_specs=vm,
        scratch_shapes=scratch,
        compiler_params=pltpu.CompilerParams(
            has_side_effects=True, vmem_limit_bytes=60 * 1024 * 1024
        ),
    )(tokens, wq, wk, wv, wg, fw.T, jnp.broadcast_to(fb[:, None], (H, 128)), wo)


def solution(mesh):
    placed = (
        P(("sp", "tp"), None),
        P(None, "tp"), P(None, "tp"), P(None, "tp"), P(None, "tp"),
        P(), P(), P(),
    )
    run = functools.partial(body, S=mesh.shape["sp"], T=mesh.shape["tp"])
    return jax.shard_map(
        run, mesh=mesh, in_specs=placed, out_specs=P(("sp", "tp"), None), check_vma=False
    )
```

```python
import functools

import jax
import jax.numpy as jnp
from jax import lax
from jax.experimental import pallas as pl
from jax.experimental.pallas import tpu as pltpu
from jax.sharding import PartitionSpec as P

HEAD_DIM = 128
CORES = 2
MESH = pl.DeviceIdType.MESH
F32 = jnp.float32
BF16 = jnp.bfloat16


def kernel(
    dims,
    x_hbm, wq_hbm, wk_hbm, wv_hbm, wg_hbm, fw_ref, fb_ref, wo_hbm,
    out_ref,
    tok, wbuf, wo, kvs, qs_, gs, fs, kvd, qd, fd, crow, obuf, oin, gin, att,
    m_ref, l_ref, acc_ref,
    load_sem, tok_send, tok_recv, tok_fwd,
    kv_send, f_send, q_send, g_send, kv_fwd, f_fwd,
    kv_recv, f_recv, q_recv, g_recv, o_send, o_recv,
):
    S, T, td, D, hd = dims
    H = T * hd
    rows = T * td
    ny = T // CORES
    gr = CORES * td
    hp = CORES * hd
    cph = S // hp
    G = CORES * cph
    seq = S * rows
    ng = S * ny
    ch = seq // (2 * G)
    qt = min(512, ch)
    kb = qt
    width = hd * HEAD_DIM
    s = lax.axis_index("sp")
    t = lax.axis_index("tp")
    y = t // CORES
    c = t % CORES
    peer = y * CORES + (1 - c)

    def remote(src, dst, ssem, rsem, ds, dt):
        return pltpu.make_async_remote_copy(
            src_ref=src, dst_ref=dst, send_sem=ssem, recv_sem=rsem,
            device_id={"sp": ds, "tp": dt}, device_id_type=MESH,
        )

    def send(src, dst, ssem, rsem, ds, dt):
        mine = jnp.logical_and(ds == s, dt == t)

        @pl.when(mine)
        def _():
            pltpu.make_async_copy(src, dst, rsem).start()

        @pl.when(jnp.logical_not(mine))
        def _():
            remote(src, dst, ssem, rsem, ds, dt).start()

    def sent(src, dst, ssem, rsem, ds, dt):
        mine = jnp.logical_and(ds == s, dt == t)

        @pl.when(jnp.logical_not(mine))
        def _():
            remote(src, dst, ssem, rsem, ds, dt).wait_send()

    def arrived(dst, rsem):
        pltpu.make_async_copy(dst, dst, rsem).wait()

    def piece(i):
        return tok.at[pl.ds(pl.multiple_of(i * td, td), td)]

    own = pltpu.make_async_copy(x_hbm, piece(t), load_sem.at[0])
    own.start()
    loads = []
    for i, w in enumerate((wk_hbm, wv_hbm, wq_hbm, wg_hbm)):
        loads.append(pltpu.make_async_copy(w, wbuf.at[i], load_sem.at[1 + i]))
    loads.append(pltpu.make_async_copy(wo_hbm, wo, load_sem.at[5]))
    for ld in loads[:4]:
        ld.start()
    barrier = pltpu.get_barrier_semaphore()
    me = s * T + t

    def greet(i, carry):
        to = lax.rem(me + i, S * T)
        pl.semaphore_signal(
            barrier, inc=1, device_id={"sp": to // T, "tp": to % T}, device_id_type=MESH
        )
        return carry

    lax.fori_loop(1, S * T, greet, 0)
    own.wait()
    pl.semaphore_wait(barrier, S * T - 1)
    tok_copies = []
    for dy in range(1, ny):
        dt = ((y + dy) % ny) * CORES + c
        tok_copies.append(remote(piece(t), piece(t), tok_send.at[dy], tok_recv.at[t], s, dt))
    tok_copies.append(remote(piece(t), piece(t), tok_send.at[0], tok_recv.at[t], s, peer))
    for cp in tok_copies:
        cp.start()
    arrived(piece(peer), tok_recv.at[peer])

    lane = lax.broadcasted_iota(jnp.int32, (H, gr), 1)
    line = lax.broadcasted_iota(jnp.int32, (H, gr), 0)
    bias = jnp.zeros((H, gr), F32)
    for h in range(H):
        bias = jnp.where(line == h, fb_ref[h], bias)

    def q_place(b):
        start = b * gr
        ci = start // ch
        late = ci // G
        r = ci + late * (2 * G - 1 - 2 * ci)
        return r, pl.multiple_of(late * ch + start % ch, gr)

    def kv_args(dy, yg, j, m):
        b = s * ny + yg
        at = (dy * hd + j) * cph + m
        j = (j + s) % hd
        jj = c * hd + j
        dst_s = jj * cph + m
        dst_t = y * CORES + s % CORES
        base = pl.multiple_of(yg * gr, gr)
        gbase = pl.multiple_of(b * gr, gr)
        return (
            (kvs.at[j, pl.ds(base, gr)], kvd.at[pl.ds(gbase, gr)], kv_send.at[at], kv_recv.at[b], dst_s, dst_t),
            (fs.at[dy, t * hd + j], fd.at[b], f_send.at[at], f_recv.at[b], dst_s, dst_t),
        )

    def q_args(dy, yg, j):
        b = s * ny + yg
        at = dy * hd + j
        j = (j + s) % hd
        jj = c * hd + j
        r, pos = q_place(b)
        base = pl.multiple_of(yg * gr, gr)
        return (
            qs_.at[j, pl.ds(base, gr)], qd.at[pl.ds(pos, gr)], q_send.at[at],
            q_recv.at[pos // gr], jj * cph + r // CORES, y * CORES + r % CORES,
        )

    def g_args(dt):
        return (
            gs.at[:, pl.ds(pl.multiple_of(dt * td, td), td)], gin.at[pl.ds(t * hd, hd)],
            g_send.at[dt], g_recv.at[t], s, dt,
        )

    for dy in range(ny):
        yg = (y + dy) % ny
        base = pl.multiple_of(yg * gr, gr)
        if dy > 0:
            got = yg * CORES + c
            other = yg * CORES + 1 - c
            arrived(piece(got), tok_recv.at[got])
            remote(piece(got), piece(got), tok_fwd.at[dy], tok_recv.at[got], s, peer).start()
            arrived(piece(other), tok_recv.at[other])
        x = tok[pl.ds(base, gr), :]
        if dy == 0:
            loads[0].wait()
        prod = jnp.dot(x, wbuf[0], preferred_element_type=F32)
        for j in range(hd):
            kvs[j, pl.ds(base, gr), 0:HEAD_DIM] = prod[:, j * HEAD_DIM : (j + 1) * HEAD_DIM].astype(BF16)
        if dy == 0:
            loads[1].wait()
        prod = jnp.dot(x, wbuf[1], preferred_element_type=F32)
        for j in range(hd):
            kvs[j, pl.ds(base, gr), HEAD_DIM:] = prod[:, j * HEAD_DIM : (j + 1) * HEAD_DIM].astype(BF16)
        logit = lax.dot_general(
            fw_ref[...], x, (((1,), (1,)), ((), ())), preferred_element_type=F32
        ) + bias
        logs = jnp.minimum(logit, 0.0) - jnp.log1p(jnp.exp(-jnp.abs(logit)))
        step = 1
        while step < gr:
            logs = logs + jnp.where(lane >= step, pltpu.roll(logs, step, 1), 0.0)
            step *= 2
        for h in range(H):
            fs[dy, h] = jnp.broadcast_to(logs[h : h + 1, :], (8, gr))
        for j in range(hd):
            for m in range(cph):
                kv, f = kv_args(dy, yg, j, m)
                send(*kv)
                send(*f)
        if dy == 0:
            loads[2].wait()
        prod = jnp.dot(x, wbuf[2], preferred_element_type=F32) * HEAD_DIM ** (-0.5)
        for j in range(hd):
            qs_[j, pl.ds(base, gr)] = prod[:, j * HEAD_DIM : (j + 1) * HEAD_DIM].astype(BF16)
        for j in range(hd):
            send(*q_args(dy, yg, j))
        if dy == 0:
            loads[3].wait()
        prod = jax.nn.sigmoid(jnp.dot(x, wbuf[3], preferred_element_type=F32))
        for j in range(hd):
            gs[j, pl.ds(base, gr)] = prod[:, j * HEAD_DIM : (j + 1) * HEAD_DIM]
        for e in range(CORES):
            send(*g_args(yg * CORES + e))
        if dy == 0:
            loads[4].start()

    def fwd_args(b):
        gbase = pl.multiple_of(b * gr, gr)
        at = (b // ny) // CORES * ny + b % ny
        blk = kvd.at[pl.ds(gbase, gr)]
        return (
            (blk, blk, kv_fwd.at[at], kv_recv.at[b], s, peer),
            (fd.at[b], fd.at[b], f_fwd.at[at], f_recv.at[b], s, peer),
        )

    def fwd_block(i, parity):
        return ((i // ny) * CORES + parity) * ny + i % ny

    def forward(i, carry):
        b = fwd_block(i, c)
        kv, f = fwd_args(b)
        arrived(f[0], f_recv.at[b])
        remote(*f).start()
        arrived(kv[0], kv_recv.at[b])
        remote(*kv).start()
        return carry

    lax.fori_loop(0, ng // CORES, forward, 0)

    def collect(i, carry):
        b = fwd_block(i, 1 - c)
        kv, f = fwd_args(b)
        arrived(f[0], f_recv.at[b])
        arrived(kv[0], kv_recv.at[b])
        return carry

    lax.fori_loop(0, ng // CORES, collect, 0)

    def q_wait(i, carry):
        arrived(qd.at[pl.ds(pl.multiple_of(i * gr, gr), gr)], q_recv.at[i])
        return carry

    lax.fori_loop(0, 2 * ch // gr, q_wait, 0)

    def chain(b, offset):
        blk = fd[b] + offset
        crow[:, pl.ds(pl.multiple_of(b * gr, gr), gr)] = blk
        return blk[:, gr - 1 : gr]

    lax.fori_loop(0, ng, chain, jnp.zeros((8, 1), F32))

    r = (s % cph) * CORES + c
    head = y * hp + s // cph
    above = lax.broadcasted_iota(jnp.int32, (qt, kb), 1) > lax.broadcasted_iota(jnp.int32, (qt, kb), 0)

    def o_args(half, u):
        ci = r if half == 0 else 2 * G - 1 - r
        token = ci * ch + u * td
        at = half * (ch // td) + u
        return (
            obuf.at[pl.ds(pl.multiple_of(half * ch + u * td, td), td)], oin.at[head],
            o_send.at[at], o_recv.at[head], token // rows, (token % rows) // td,
        )

    for half in range(2):
        ci = r if half == 0 else 2 * G - 1 - r
        for tile in range(ch // qt):
            at = half * ch + tile * qt
            q0 = pl.multiple_of(ci * ch + tile * qt, qt)
            q = qd[at : at + qt, :]
            cq = crow[:, pl.ds(q0, qt)]
            c0 = cq[0:1, 0:1]
            cqc = (cq - c0).T[:, 0:1]
            m_ref[...] = jnp.full(m_ref.shape, -1e30, F32)
            l_ref[...] = jnp.zeros(l_ref.shape, F32)
            acc_ref[...] = jnp.zeros(acc_ref.shape, F32)

            def absorb(kblk, masked, q=q, c0=c0, cqc=cqc):
                k0 = pl.multiple_of(kblk * kb, kb)
                scores = lax.dot_general(
                    q, kvd[pl.ds(k0, kb), 0:HEAD_DIM], (((1,), (1,)), ((), ())),
                    preferred_element_type=F32,
                )
                scores = scores + (c0 - crow[0:1, pl.ds(k0, kb)])
                if masked:
                    scores = jnp.where(above, -jnp.inf, scores)
                best = m_ref[:, 0:1]
                top = jnp.maximum(best, jnp.max(scores, axis=1, keepdims=True) + cqc)
                factor = jnp.exp(best - top)
                weights = jnp.exp(scores - (top - cqc))
                part = weights[:, 0:128]
                for i in range(1, kb // 128):
                    part = part + weights[:, i * 128 : (i + 1) * 128]
                l_ref[...] = l_ref[...] * factor + part
                acc_ref[...] = acc_ref[...] * factor + jnp.dot(
                    weights.astype(BF16), kvd[pl.ds(k0, kb), HEAD_DIM:], preferred_element_type=F32
                )
                m_ref[...] = jnp.broadcast_to(top, m_ref.shape)

            full = q0 // kb

            def full_step(i, carry):
                absorb(i, False)
                return carry

            lax.fori_loop(0, full, full_step, 0)
            absorb(full, True)
            total = jnp.sum(l_ref[...], axis=1, keepdims=True)
            obuf[at : at + qt, :] = (acc_ref[...] / total).astype(BF16)
            for u in range(qt // td):
                send(*o_args(half, tile * (qt // td) + u))

    def g_wait(i, carry):
        arrived(gin.at[pl.ds(i * hd, hd)], g_recv.at[i])
        return carry

    lax.fori_loop(0, T, g_wait, 0)
    loads[4].wait()
    for h in range(H):
        arrived(oin.at[h], o_recv.at[h])
        att[:, h * HEAD_DIM : (h + 1) * HEAD_DIM] = (oin[h].astype(F32) * gin[h]).astype(BF16)
    cols = 512
    for n in range(D // cols):
        out_ref[:, n * cols : (n + 1) * cols] = jnp.dot(
            att[...], wo[:, n * cols : (n + 1) * cols], preferred_element_type=F32
        ).astype(BF16)

    for cp in tok_copies:
        cp.wait_send()
    for dy in range(ny):
        yg = (y + dy) % ny
        if dy > 0:
            got = yg * CORES + c
            remote(piece(got), piece(got), tok_fwd.at[dy], tok_recv.at[got], s, peer).wait_send()
        for j in range(hd):
            for m in range(cph):
                kv, f = kv_args(dy, yg, j, m)
                sent(*kv)
                sent(*f)
            sent(*q_args(dy, yg, j))
        for e in range(CORES):
            sent(*g_args(yg * CORES + e))

    def fwd_done(i, carry):
        kv, f = fwd_args(fwd_block(i, c))
        remote(*f).wait_send()
        remote(*kv).wait_send()
        return carry

    lax.fori_loop(0, ng // CORES, fwd_done, 0)
    for half in range(2):
        for u in range(ch // td):
            sent(*o_args(half, u))


def body(tokens, wq, wk, wv, wg, fw, fb, wo, *, S, T):
    td, D = tokens.shape
    width = wq.shape[1]
    hd = width // HEAD_DIM
    H = T * hd
    rows = T * td
    ny = T // CORES
    gr = CORES * td
    hp = CORES * hd
    cph = S // hp
    G = CORES * cph
    seq = S * rows
    ng = S * ny
    ch = seq // (2 * G)
    qt = min(512, ch)
    dma = pltpu.SemaphoreType.DMA
    vmem = pltpu.VMEM
    any_ = pl.BlockSpec(memory_space=pl.ANY)
    vm = pl.BlockSpec(memory_space=pltpu.VMEM)
    smem = pl.BlockSpec(memory_space=pltpu.SMEM)
    scratch = [
        vmem((rows, D), BF16), vmem((4, D, width), BF16), vmem((D, D), BF16),
        vmem((hd, rows, 2 * HEAD_DIM), BF16), vmem((hd, rows, HEAD_DIM), BF16),
        vmem((hd, rows, HEAD_DIM), F32), vmem((ny, H, 8, gr), F32),
        vmem((seq, 2 * HEAD_DIM), BF16), vmem((2 * ch, HEAD_DIM), BF16),
        vmem((ng, 8, gr), F32), vmem((8, seq), F32), vmem((2 * ch, HEAD_DIM), BF16),
        vmem((H, td, HEAD_DIM), BF16), vmem((H, td, HEAD_DIM), F32), vmem((td, D), BF16),
        vmem((qt, 128), F32), vmem((qt, 128), F32), vmem((qt, HEAD_DIM), F32),
        dma((6,)), dma((ny,)), dma((T,)), dma((ny,)),
        dma((ny * hd * cph,)), dma((ny * hd * cph,)), dma((ny * hd,)), dma((T,)),
        dma((ng // CORES,)), dma((ng // CORES,)),
        dma((ng,)), dma((ng,)), dma((2 * ch // gr,)), dma((T,)), dma((2 * ch // td,)), dma((H,)),
    ]
    return pl.pallas_call(
        functools.partial(kernel, (S, T, td, D, hd)),
        out_shape=jax.ShapeDtypeStruct((td, D), BF16),
        in_specs=[any_, any_, any_, any_, any_, vm, smem, any_],
        out_specs=vm,
        scratch_shapes=scratch,
        compiler_params=pltpu.CompilerParams(
            has_side_effects=True, collective_id=0, vmem_limit_bytes=60 * 1024 * 1024
        ),
    )(tokens, wq, wk, wv, wg, fw.T, fb, wo)


def solution(mesh):
    placed = (
        P(("sp", "tp"), None),
        P(None, "tp"), P(None, "tp"), P(None, "tp"), P(None, "tp"),
        P(), P(), P(),
    )
    run = functools.partial(body, S=mesh.shape["sp"], T=mesh.shape["tp"])
    return jax.shard_map(
        run, mesh=mesh, in_specs=placed, out_specs=P(("sp", "tp"), None), check_vma=False
    )
```
